32 devices in a mesh: grp: 2 (over x), tp: 16 (over z, y, core).
Axes of the slice: x: 2, y: 2, z: 4, core: 2. Of those that a mesh axis runs over, the one named last changes fastest.
Arguments:
- residual_channel: bfloat16 [256, 8, 4096], P('grp', None, 'tp'), parts along dimension 0, may hold values from -18 to 18, as said below
- prior_block_multiplier: float32 [2, 4096], replicated, may hold values from 0.1 to 1.9
- probe_map_matrix: bfloat16 [2, 4096, 2048], P(None, None, 'tp'), may hold values from -0.09375 to 0.09375
- lookup_map_matrix: bfloat16 [2, 4096, 2048], P(None, None, 'tp'), may hold values from -0.09375 to 0.09375
- content_map_matrix: bfloat16 [2, 4096, 2048], P(None, None, 'tp'), may hold values from -0.09375 to 0.09375
- emission_valve_matrix: bfloat16 [2, 4096, 2048], P(None, None, 'tp'), may hold values from -0.09375 to 0.09375
- forgetting_map_matrix: bfloat16 [2, 4096, 32], replicated, may hold values from -0.09375 to 0.09375
- insertion_rate_matrix: bfloat16 [2, 4096, 32], replicated, may hold values from -0.09375 to 0.09375
- forgetting_magnitude_exponent: float32 [2, 32], P(None, 'tp'), may hold values from -4.6 to -1.2
- channel_forgetting_offset: float32 [2, 32], P(None, 'tp'), may hold values from -2 to 1
- surplus_forgetting_amounts: float32 [2, 256, 8, 32], P(None, 'grp', None, 'tp'), parts along dimension 1, may hold values from -0.7 to 0
- readout_rescale_multiplier: float32 [2, 2048], P(None, 'tp'), may hold values from 0.1 to 1.9
- emission_map_matrix: bfloat16 [2, 2048, 4096], P(None, None, 'tp'), may hold values from -2 to 2
- post_mixing_multiplier: float32 [2, 4096], replicated, may hold values from 0.1 to 1.9
- recurrent_matrices: float32 [2, 256, 32, 4096], P(None, 'grp', 'tp'), parts along dimension 1, may hold values from -6 to 6
Outputs:
- new_stream: bfloat16 [256, 8, 4096], P('grp', None, 'tp'), parts along dimension 0
- new_memory: float32 [2, 256, 32, 4096], P(None, 'grp', 'tp'), parts along dimension 1
The draws below stay inside these ranges and needn't reach their ends.
There are 2 independent parts, one for each index of `grp`. The reference program is written for one: setup_inputs(seed, part) draws one part's arguments, and reference() takes and returns one part's arrays. A program takes and returns all parts, laid end to end along the dimension named above; an argument that names none is the same for every part. Nothing has to cross between parts.
Inputs may be any that keep to these rules, and one draw needn't show every extreme that they name: `residual_channel`: column scales of the features differ widely.
All inputs are finite; a program needn't handle non-finite values.
Results may differ from the reference program's by a relative error of at most 0.0081.
Values may be sent and summed in bfloat16 or wider, within the bound.
A program may use at most 192 MiB of HBM per device.

```python
import math
import jax
import jax.numpy as jnp
from jax import lax

D = 4096
HEADS = 32
HEAD_DIM = 64
LAYERS = 2
STEPS = 8
SEQS = 128
MIXW = 2048


def column_scales(key, count):
    ramp = jnp.exp(math.log(0.4) + math.log(8.0) * jnp.arange(count, dtype=jnp.float32) / count)
    return ramp * jax.random.uniform(key, (count,), jnp.float32, 0.6, 1.4)


def draw_residual_channel(key, part):
    key_cols = jax.random.fold_in(key, 11)
    key_vals = jax.random.fold_in(key, 12)
    columns = column_scales(key_cols, D)
    entries = jnp.clip(jax.random.normal(key_vals, (SEQS, STEPS, D), jnp.float32), -4.0, 4.0)
    return (entries * columns).astype(jnp.bfloat16)


def draw_emission_map_matrix(key, part):
    key_cols = jax.random.fold_in(key, 21)
    key_vals = jax.random.fold_in(key, 22)
    columns = column_scales(key_cols, D)
    entries = jnp.clip(jax.random.normal(key_vals, (LAYERS, MIXW, D), jnp.float32), -3.0, 3.0)
    return (entries * columns * MIXW ** (-0.5)).astype(jnp.bfloat16)


def draw_surplus_forgetting_amounts(key, part):
    key_mask = jax.random.fold_in(key, 31)
    key_depth = jax.random.fold_in(key, 32)
    chosen = jax.random.bernoulli(key_mask, 0.12, (LAYERS, SEQS, STEPS, HEADS))
    depth = jax.random.uniform(key_depth, (LAYERS, SEQS, STEPS, HEADS), jnp.float32, math.log(0.5), math.log(0.8))
    return jnp.where(chosen, depth, 0.0).astype(jnp.float32)


def level_of(key, extent, pieces, least, largest):
    level = 1.0
    for dim, shards_of in pieces:
        heights = jax.random.uniform(jax.random.fold_in(jax.random.fold_in(key, 6), dim), (shards_of,), jnp.float32, least / len(pieces), largest / len(pieces))
        level = level * jnp.repeat(jnp.exp(heights), extent[dim] // shards_of).reshape((-1,) + (1,) * (len(extent) - 1 - dim))
    return level


def normal_values(stream_key, shape, width, bound, split=(), held_as=jnp.bfloat16):
    gain = level_of(stream_key, shape, split, -0.22, 0.18) if split else 1.0
    result = jax.random.normal(stream_key, shape, jnp.float32) * width * gain
    return jnp.minimum(jnp.maximum(result, -bound), bound).astype(held_as)


def setup_inputs(seed: int = 0, part: int = 0) -> dict:
    key_of = jax.random.split(jax.random.key(seed), 16)
    own_keys = jax.random.split(jax.random.fold_in(key_of[15], part), 16)
    return {
        "residual_channel": draw_residual_channel(jax.random.fold_in(jax.random.fold_in(key_of[15], part), 71), part),
        "prior_block_multiplier": jnp.clip(1.0 + 0.18 * jax.random.normal(key_of[1], (LAYERS, D), jnp.float32), 0.1, 1.9),
        "probe_map_matrix": normal_values(key_of[2], (LAYERS, D, MIXW), D ** -0.5, 0.09375, ((2, 16),)),
        "lookup_map_matrix": normal_values(key_of[3], (LAYERS, D, MIXW), D ** -0.5, 0.09375, ((2, 16),)),
        "content_map_matrix": normal_values(key_of[4], (LAYERS, D, MIXW), D ** -0.5, 0.09375, ((2, 16),)),
        "emission_valve_matrix": normal_values(key_of[5], (LAYERS, D, MIXW), D ** -0.5, 0.09375, ((2, 16),)),
        "forgetting_map_matrix": normal_values(key_of[6], (LAYERS, D, HEADS), D ** -0.5, 0.09375),
        "insertion_rate_matrix": normal_values(key_of[7], (LAYERS, D, HEADS), D ** -0.5, 0.09375),
        "forgetting_magnitude_exponent": jnp.clip(-4.6 + 3.3999999 * jax.random.uniform(key_of[8], (LAYERS, HEADS), jnp.float32) ** level_of(key_of[8], (LAYERS, HEADS), ((1, 16),), -0.2, 0.2), -4.6, -1.2),
        "channel_forgetting_offset": jnp.clip(-2.0 + 3.0 * jax.random.uniform(key_of[9], (LAYERS, HEADS), jnp.float32) ** level_of(key_of[9], (LAYERS, HEADS), ((1, 16),), -0.2, 0.2), -2.0, 1.0),
        "surplus_forgetting_amounts": draw_surplus_forgetting_amounts(jax.random.fold_in(jax.random.fold_in(key_of[15], part), 71), part),
        "readout_rescale_multiplier": jnp.clip(1.0 + 0.18 * jax.random.normal(key_of[11], (LAYERS, MIXW), jnp.float32), 0.1, 1.9),
        "emission_map_matrix": draw_emission_map_matrix(jax.random.fold_in(key_of[15], 71), part),
        "post_mixing_multiplier": jnp.clip(1.0 + 0.18 * jax.random.normal(key_of[13], (LAYERS, D), jnp.float32), 0.1, 1.9),
        "recurrent_matrices": normal_values(own_keys[14], (LAYERS, SEQS, HEADS, HEAD_DIM * HEAD_DIM), 1.0, 6.0, ((2, 16),), jnp.float32),
    }


EPS = 1e-06
HIGH = lax.Precision.HIGHEST

def solve_lower(a_mat, right_side):
    length = right_side.shape[-2]
    solved_rows = []
    for row_at in range(length):
        current_row = right_side[..., row_at, :]
        for col_at in range(row_at):
            current_row = current_row - a_mat[..., row_at, col_at][..., None] * solved_rows[col_at]
        solved_rows.append(current_row)
    return jnp.stack(solved_rows, axis=-2)

def delta_block(queries, key_rows, values, forgetting_exponent_amount, strength, matrix_state):
    length = queries.shape[2]
    causal = jnp.tril(jnp.ones((length, length), bool))
    strict = jnp.tril(jnp.ones((length, length), bool), -1)
    cumulative = jnp.cumsum(forgetting_exponent_amount, axis=-1)
    decay_mat = jnp.where(causal, jnp.exp(jnp.where(causal, cumulative[..., :, None] - cumulative[..., None, :], 0.0)), 0.0)
    key_gram = jnp.einsum('bhtd,bhsd->bhts', key_rows, key_rows, precision=HIGH)
    a_mat = jnp.where(strict, strength[..., :, None] * decay_mat * key_gram, 0.0)
    right_side = jnp.concatenate([strength[..., None] * values, (strength * jnp.exp(cumulative))[..., None] * key_rows], axis=-1)
    solved = solve_lower(a_mat, right_side)
    width_v = values.shape[-1]
    update = solved[..., :width_v] - jnp.einsum('bhtk,bhkv->bhtv', solved[..., width_v:], matrix_state, precision=HIGH)
    scores = jnp.einsum('bhtd,bhsd->bhts', queries, key_rows, precision=HIGH) * decay_mat
    output = jnp.exp(cumulative)[..., None] * jnp.einsum('bhtk,bhkv->bhtv', queries, matrix_state, precision=HIGH)
    output = output + jnp.einsum('bhts,bhsv->bhtv', scores, update, precision=HIGH)
    final_log = cumulative[..., -1:]
    revised_memory_matrix = jnp.exp(final_log)[..., None] * matrix_state + jnp.einsum('bhsk,bhsv->bhkv', key_rows * jnp.exp(final_log - cumulative)[..., None], update, precision=HIGH)
    return (output, revised_memory_matrix)

def unit_rows(matrix):
    return matrix * lax.rsqrt(lax.optimization_barrier(jnp.sum(matrix * matrix, axis=-1, keepdims=True)) + EPS)

def token_blender(mapped_token_vectors, magnitude_exponent, offset_terms_array, surplus_forgetting_exponent, multiplier_terms_array, incoming_memory_matrix, batch_total, generation_round_total):
    rounded = [lax.optimization_barrier(part_sum.astype(jnp.bfloat16)).astype(jnp.float32) for part_sum in mapped_token_vectors]
    queries, keys_raw, values_raw, gate_raw, decay_pre, strength_pre = rounded
    head_count = incoming_memory_matrix.shape[1]

    def to_heads(matrix):
        return matrix.reshape(batch_total, generation_round_total, head_count, HEAD_DIM).transpose(0, 2, 1, 3)

    def per_head(matrix):
        return matrix.reshape(batch_total, generation_round_total, head_count).transpose(0, 2, 1)
    queries = unit_rows(jax.nn.silu(to_heads(queries))) * HEAD_DIM ** (-0.5)
    key_rows = unit_rows(jax.nn.silu(to_heads(keys_raw)))
    values = jax.nn.silu(to_heads(values_raw))
    forgetting_exponent_amount = -jnp.exp(magnitude_exponent)[None, :, None] * jax.nn.softplus(per_head(decay_pre) + offset_terms_array[None, :, None])
    forgetting_exponent_amount = forgetting_exponent_amount + surplus_forgetting_exponent.transpose(0, 2, 1)
    strength = jax.nn.sigmoid(per_head(strength_pre))
    matrix_state = incoming_memory_matrix.reshape(batch_total, head_count, HEAD_DIM, HEAD_DIM)
    output, revised_memory_matrix = delta_block(queries, key_rows, values, forgetting_exponent_amount, strength, matrix_state)
    normed = output * lax.rsqrt(lax.optimization_barrier(jnp.mean(output * output, axis=-1, keepdims=True)) + EPS)
    normed = normed * multiplier_terms_array.reshape(head_count, HEAD_DIM)[None, :, None, :] * jax.nn.silu(to_heads(gate_raw))
    blended_token_vectors = normed.transpose(0, 2, 1, 3).reshape(batch_total * generation_round_total, head_count * HEAD_DIM).astype(jnp.bfloat16)
    return (blended_token_vectors, revised_memory_matrix.reshape(batch_total, head_count, HEAD_DIM * HEAD_DIM))

def reference(residual_channel, prior_block_multiplier, probe_map_matrix, lookup_map_matrix, content_map_matrix, emission_valve_matrix, forgetting_map_matrix, insertion_rate_matrix, forgetting_magnitude_exponent, channel_forgetting_offset, surplus_forgetting_amounts, readout_rescale_multiplier, emission_map_matrix, post_mixing_multiplier, recurrent_matrices):
    batch_total, generation_round_total = (residual_channel.shape[0], residual_channel.shape[1])
    current = residual_channel.reshape(batch_total * generation_round_total, D)
    states = []
    for block_index_number in range(LAYERS):
        widened = current.astype(jnp.float32)
        inv_rms = lax.rsqrt(lax.optimization_barrier(jnp.mean(widened * widened, axis=-1, keepdims=True)) + EPS)
        hidden = (widened * inv_rms * prior_block_multiplier[block_index_number]).astype(jnp.bfloat16)
        mapped_token_vectors = tuple((jnp.dot(hidden, weight[block_index_number], preferred_element_type=jnp.float32) for weight in (probe_map_matrix, lookup_map_matrix, content_map_matrix, emission_valve_matrix, forgetting_map_matrix, insertion_rate_matrix)))
        blended_token_vectors, revised_memory_matrix = token_blender(mapped_token_vectors, forgetting_magnitude_exponent[block_index_number], channel_forgetting_offset[block_index_number], surplus_forgetting_amounts[block_index_number], readout_rescale_multiplier[block_index_number], recurrent_matrices[block_index_number], batch_total, generation_round_total)
        mixed_out = jnp.dot(blended_token_vectors, emission_map_matrix[block_index_number], preferred_element_type=jnp.float32).astype(jnp.bfloat16)
        mixed_wide = lax.optimization_barrier(mixed_out).astype(jnp.float32)
        post_rms = lax.rsqrt(lax.optimization_barrier(jnp.mean(mixed_wide * mixed_wide, axis=-1, keepdims=True)) + EPS)
        current = lax.optimization_barrier((widened + mixed_wide * post_rms * post_mixing_multiplier[block_index_number]).astype(jnp.bfloat16))
        states.append(revised_memory_matrix)
    return (current.reshape(batch_total, generation_round_total, D), jnp.stack(states, axis=0))
```

```python
import jax
import jax.numpy as jnp
from jax import lax
from jax.experimental import pallas as pl
from jax.experimental.pallas import tpu as pltpu
from jax.sharding import PartitionSpec as P

D = 4096
HEAD_DIM = 64
LAYERS = 2


EPS = 1e-06
HIGH = lax.Precision.HIGHEST


def solve_lower(a_mat, right_side):
    length = right_side.shape[-2]
    solved_rows = []
    for row_at in range(length):
        current_row = right_side[..., row_at, :]
        for col_at in range(row_at):
            current_row = current_row - a_mat[..., row_at, col_at][..., None] * solved_rows[col_at]
        solved_rows.append(current_row)
    return jnp.stack(solved_rows, axis=-2)


def delta_block(queries, key_rows, values, forgetting_exponent_amount, strength, matrix_state):
    length = queries.shape[2]
    causal = jnp.tril(jnp.ones((length, length), bool))
    strict = jnp.tril(jnp.ones((length, length), bool), -1)
    cumulative = jnp.cumsum(forgetting_exponent_amount, axis=-1)
    decay_mat = jnp.where(
        causal,
        jnp.exp(jnp.where(causal, cumulative[..., :, None] - cumulative[..., None, :], 0.0)),
        0.0,
    )
    key_gram = jnp.einsum("bhtd,bhsd->bhts", key_rows, key_rows, precision=HIGH)
    a_mat = jnp.where(strict, strength[..., :, None] * decay_mat * key_gram, 0.0)
    right_side = jnp.concatenate(
        [strength[..., None] * values, (strength * jnp.exp(cumulative))[..., None] * key_rows],
        axis=-1,
    )
    solved = solve_lower(a_mat, right_side)
    width_v = values.shape[-1]
    update = solved[..., :width_v] - jnp.einsum(
        "bhtk,bhkv->bhtv", solved[..., width_v:], matrix_state, precision=HIGH
    )
    scores = jnp.einsum("bhtd,bhsd->bhts", queries, key_rows, precision=HIGH) * decay_mat
    output = jnp.exp(cumulative)[..., None] * jnp.einsum(
        "bhtk,bhkv->bhtv", queries, matrix_state, precision=HIGH
    )
    output = output + jnp.einsum("bhts,bhsv->bhtv", scores, update, precision=HIGH)
    final_log = cumulative[..., -1:]
    revised_memory_matrix = jnp.exp(final_log)[..., None] * matrix_state + jnp.einsum(
        "bhsk,bhsv->bhkv",
        key_rows * jnp.exp(final_log - cumulative)[..., None],
        update,
        precision=HIGH,
    )
    return (output, revised_memory_matrix)


def unit_rows(matrix):
    return matrix * lax.rsqrt(jnp.sum(matrix * matrix, axis=-1, keepdims=True) + EPS)


def token_blender(
    mapped_token_vectors,
    magnitude_exponent,
    offset_terms_array,
    surplus_forgetting_exponent,
    multiplier_terms_array,
    incoming_memory_matrix,
    batch_total,
    generation_round_total,
):
    rounded = [
        lax.optimization_barrier(part_sum.astype(jnp.bfloat16)).astype(jnp.float32)
        for part_sum in mapped_token_vectors
    ]
    queries, keys_raw, values_raw, gate_raw, decay_pre, strength_pre = rounded
    head_count = incoming_memory_matrix.shape[1]

    def to_heads(matrix):
        return matrix.reshape(batch_total, generation_round_total, head_count, HEAD_DIM).transpose(
            0, 2, 1, 3
        )

    def per_head(matrix):
        return matrix.reshape(batch_total, generation_round_total, head_count).transpose(0, 2, 1)

    queries = unit_rows(jax.nn.silu(to_heads(queries))) * HEAD_DIM ** (-0.5)
    key_rows = unit_rows(jax.nn.silu(to_heads(keys_raw)))
    values = jax.nn.silu(to_heads(values_raw))
    forgetting_exponent_amount = -jnp.exp(magnitude_exponent)[None, :, None] * jax.nn.softplus(
        per_head(decay_pre) + offset_terms_array[None, :, None]
    )
    forgetting_exponent_amount = forgetting_exponent_amount + surplus_forgetting_exponent.transpose(
        0, 2, 1
    )
    strength = jax.nn.sigmoid(per_head(strength_pre))
    matrix_state = incoming_memory_matrix.reshape(batch_total, head_count, HEAD_DIM, HEAD_DIM)
    output, revised_memory_matrix = delta_block(
        queries, key_rows, values, forgetting_exponent_amount, strength, matrix_state
    )
    normed = output * lax.rsqrt(jnp.mean(output * output, axis=-1, keepdims=True) + EPS)
    normed = (
        normed
        * multiplier_terms_array.reshape(head_count, HEAD_DIM)[None, :, None, :]
        * jax.nn.silu(to_heads(gate_raw))
    )
    blended_token_vectors = (
        normed.transpose(0, 2, 1, 3)
        .reshape(batch_total * generation_round_total, head_count * HEAD_DIM)
        .astype(jnp.bfloat16)
    )
    return (
        blended_token_vectors,
        revised_memory_matrix.reshape(batch_total, head_count, HEAD_DIM * HEAD_DIM),
    )


LANES = 128


def bf16_dot(left, right):
    return jnp.dot(left, right, preferred_element_type=jnp.float32)


def head_sums(squares, ones):
    high = squares.astype(jnp.bfloat16)
    low = (squares - high.astype(jnp.float32)).astype(jnp.bfloat16)
    return bf16_dot(high, ones) + bf16_dot(low, ones)


def mixer_kernel(
    proj_ref, surplus_ref, vec_ref, spread_ref, ones_ref, perm_ref, state_ref, *rest
):
    y_ref, new_ref, qk_ref, x_ref, kd_ref, u_ref, qs_ref, dec_ref = rest[-8:]
    rows = proj_ref.shape[0]
    seqs, steps = qk_ref.shape[1], qk_ref.shape[2]
    f32, bf16 = jnp.float32, jnp.bfloat16
    ones = ones_ref[...]
    perm = perm_ref[...]

    def cols(at):
        return proj_ref[:, at * LANES : (at + 1) * LANES].astype(f32)

    def tokens(matrix):
        return matrix.reshape(seqs, steps, LANES)

    queries = jax.nn.silu(cols(0))
    keys = jax.nn.silu(cols(1))
    sums = head_sums(jnp.concatenate([queries * queries, keys * keys], axis=1), ones)
    queries = tokens(queries * lax.rsqrt(sums[:, :LANES] + EPS) * HEAD_DIM ** (-0.5))
    keys = tokens(keys * lax.rsqrt(sums[:, LANES:] + EPS))
    spread = bf16_dot(proj_ref[:, 4 * LANES : 5 * LANES], spread_ref[...])
    biased = spread[:, :LANES] + vec_ref[1:2, :]
    softplus = jnp.maximum(biased, 0.0) + jnp.log1p(jnp.exp(-jnp.abs(biased)))
    cumulative = tokens(vec_ref[0:1, :] * softplus + surplus_ref[...])
    beta = tokens(jax.nn.sigmoid(spread[:, LANES:]))
    token = lax.broadcasted_iota(jnp.int32, (seqs, steps, LANES), 1)
    shift = 1
    while shift < steps:
        moved = pltpu.roll(cumulative, shift, axis=1)
        cumulative = cumulative + jnp.where(token >= shift, moved, 0.0)
        shift *= 2
    grown = jnp.exp(cumulative)
    solved_u = beta * tokens(jax.nn.silu(cols(2)))
    solved_p = beta * grown * keys
    for at in range(steps):
        causal = token >= at
        gap = jnp.where(causal, cumulative - cumulative[:, at : at + 1, :], 0.0)
        decay = jnp.where(causal, jnp.exp(gap), 0.0)
        key_row = keys[:, at : at + 1, :]
        pair = jnp.concatenate([queries * key_row, keys * key_row], axis=2)
        dots = bf16_dot(pair.reshape(rows, 2 * LANES).astype(bf16), ones)
        qk_ref[at] = tokens(dots[:, :LANES]) * decay
        if at < steps - 1:
            a_col = jnp.where(token > at, beta * decay * tokens(dots[:, LANES:]), 0.0)
            solved_u = solved_u - a_col * solved_u[:, at : at + 1, :]
            solved_p = solved_p - a_col * solved_p[:, at : at + 1, :]
    last = cumulative[:, steps - 1 : steps, :]
    faded = keys * jnp.exp(last - cumulative)

    def permuted(first, second):
        both = jnp.concatenate([first, second], axis=1).reshape(2 * rows, LANES)
        return bf16_dot(both.astype(bf16), perm).astype(bf16).reshape(seqs, 2 * steps, LANES)

    x_ref[...] = permuted(queries, solved_p)
    kd_ref[...] = permuted(faded, faded)
    u_ref[...] = solved_u
    dec_ref[...] = jnp.broadcast_to(jnp.exp(last), (seqs, steps, LANES))

    state_rows = state_ref.shape[2]
    even = lax.broadcasted_iota(jnp.int32, (state_rows, LANES), 0) % 2 == 0
    left = lax.broadcasted_iota(jnp.int32, (state_rows, LANES), 1) < HEAD_DIM
    kept = even == left

    def one_sequence(at, carry):
        state = state_ref[0, at]
        turned = pltpu.roll(state, HEAD_DIM, axis=1)
        upper = jnp.where(kept, jnp.where(even, state, turned), 0.0)
        lower = jnp.where(kept, jnp.where(even, turned, state), 0.0)
        wide = jnp.concatenate([upper, lower], axis=0).astype(bf16)
        read = bf16_dot(x_ref[at], wide)
        qs_ref[at] = read[:steps]
        update = u_ref[at] - read[steps:]
        u_ref[at] = update
        high = update.astype(bf16).astype(f32)
        split = jnp.concatenate([high, update - high], axis=0).astype(bf16)
        grow = lax.dot_general(
            kd_ref[at], split, (((0,), (0,)), ((), ())), preferred_element_type=f32
        )
        grow_0, grow_1 = grow[:state_rows], grow[state_rows:]
        crossed = pltpu.roll(jnp.where(even, grow_1, grow_0), HEAD_DIM, axis=1)
        added = jnp.where(kept, jnp.where(even, grow_0, grow_1), crossed)
        fade = dec_ref[at]
        fade_turned = pltpu.roll(fade, HEAD_DIM, axis=1)
        copies = state_rows // steps
        factor = jnp.where(
            kept,
            jnp.concatenate([fade] * copies, axis=0),
            jnp.concatenate([fade_turned] * copies, axis=0),
        )
        new_ref[0, at] = factor * state + added
        return carry

    lax.fori_loop(0, seqs, one_sequence, 0, unroll=4)
    update = u_ref[...]
    output = grown * qs_ref[...]
    for at in range(steps):
        output = output + qk_ref[at] * update[:, at : at + 1, :]
    output = output.reshape(rows, LANES)
    squares = head_sums(output * output, ones[:LANES, :LANES])
    output = output * lax.rsqrt(squares * (1.0 / HEAD_DIM) + EPS)
    y_ref[...] = (output * vec_ref[2:3, :] * jax.nn.silu(cols(3))).astype(bf16)


def mixer_constants(head_count):
    row = jnp.arange(2 * LANES)[:, None]
    col = jnp.arange(2 * LANES)[None, :]
    ones = (row // HEAD_DIM == col // HEAD_DIM).astype(jnp.bfloat16)
    spread = (row[:LANES] == col // HEAD_DIM).astype(jnp.bfloat16)
    head, channel = row[:LANES] // HEAD_DIM, row[:LANES] % HEAD_DIM
    target = (channel % 2) * HEAD_DIM + (channel // 2) * head_count + head
    perm = (target == col[:, :LANES]).astype(jnp.bfloat16)
    return spread, ones, perm


def mixer(proj, surplus, vectors, constants, states, layer, earlier):
    rows = proj.shape[0]
    layers, all_seqs, state_rows, _ = states.shape
    seqs_here = all_seqs
    steps = rows // seqs_here
    block = next(size for size in (32, 16, 8, 4, 2, 1) if seqs_here % size == 0)
    token_rows = block * steps
    spread, ones, perm = constants

    def whole(array):
        return pl.BlockSpec(array.shape, lambda i: (0,) * array.ndim)

    in_specs = [
        pl.BlockSpec((token_rows, proj.shape[1]), lambda i: (i, 0)),
        pl.BlockSpec((token_rows, LANES), lambda i: (i, 0)),
        whole(vectors),
        whole(spread),
        whole(ones),
        whole(perm),
        pl.BlockSpec((1, block, state_rows, LANES), lambda i: (layer, i, 0, 0)),
    ]
    operands = [proj, surplus, vectors, spread, ones, perm, states]
    aliases = {}
    if earlier is not None:
        in_specs.append(pl.BlockSpec(memory_space=pl.ANY))
        operands.append(earlier)
        aliases = {len(operands) - 1: 1}
    tile = (block, steps, LANES)
    return pl.pallas_call(
        mixer_kernel,
        grid=(seqs_here // block,),
        in_specs=in_specs,
        out_specs=[
            pl.BlockSpec((token_rows, LANES), lambda i: (i, 0)),
            pl.BlockSpec((1, block, state_rows, LANES), lambda i: (layer, i, 0, 0)),
        ],
        out_shape=[
            jax.ShapeDtypeStruct((rows, LANES), jnp.bfloat16),
            jax.ShapeDtypeStruct(states.shape, jnp.float32),
        ],
        scratch_shapes=[
            pltpu.VMEM((steps,) + tile, jnp.float32),
            pltpu.VMEM((block, 2 * steps, LANES), jnp.bfloat16),
            pltpu.VMEM((block, 2 * steps, LANES), jnp.bfloat16),
            pltpu.VMEM(tile, jnp.float32),
            pltpu.VMEM(tile, jnp.float32),
            pltpu.VMEM(tile, jnp.float32),
        ],
        input_output_aliases=aliases,
        cost_estimate=pl.CostEstimate(
            flops=rows * 20 * 2 * LANES * 2 * LANES,
            bytes_accessed=2 * all_seqs * state_rows * LANES * 4,
            transcendentals=rows * LANES * 12,
        ),
        name="mixer",
    )(*operands)


def project(portion, weights):
    return tuple(
        (jnp.dot(portion, weight, preferred_element_type=jnp.float32) for weight in weights)
    )


def out_project(blended_token_vectors, weight_rows):
    return jnp.dot(
        lax.all_gather(blended_token_vectors, "tp", axis=1, tiled=True),
        weight_rows,
        preferred_element_type=jnp.float32,
    ).astype(jnp.bfloat16)


def post_residual(widened, mixed_out, multiplier_terms_array, complete):
    mixed_wide = lax.optimization_barrier(mixed_out).astype(jnp.float32)
    squares = jnp.sum(mixed_wide * mixed_wide, axis=-1)
    if not complete:
        squares = lax.psum(squares, "tp")
    post_rms = lax.rsqrt(squares / D + EPS)[:, None]
    return lax.optimization_barrier(
        (widened + mixed_wide * post_rms * multiplier_terms_array).astype(jnp.bfloat16)
    )


def local(
    residual_channel,
    prior_block_multiplier,
    probe_map_matrix,
    lookup_map_matrix,
    content_map_matrix,
    emission_valve_matrix,
    forgetting_map_matrix,
    insertion_rate_matrix,
    forgetting_magnitude_exponent,
    channel_forgetting_offset,
    surplus_forgetting_amounts,
    readout_rescale_multiplier,
    emission_map_matrix,
    post_mixing_multiplier,
    recurrent_matrices,
):
    batch_total, generation_round_total, own_width = residual_channel.shape
    head_count = recurrent_matrices.shape[2]
    row_count = batch_total * generation_round_total
    col_offset = lax.axis_index("tp") * own_width
    head_offset = lax.axis_index("tp") * head_count
    new_states = []

    def mix_layer(mapped_token_vectors, block_index_number):
        blended_token_vectors, revised_memory_matrix = token_blender(
            mapped_token_vectors,
            forgetting_magnitude_exponent[block_index_number],
            channel_forgetting_offset[block_index_number],
            surplus_forgetting_amounts[block_index_number],
            readout_rescale_multiplier[block_index_number],
            recurrent_matrices[block_index_number],
            batch_total,
            generation_round_total,
        )
        new_states.append(revised_memory_matrix)
        return out_project(blended_token_vectors, emission_map_matrix[block_index_number])

    def own_cols(matrix):
        return lax.dynamic_slice_in_dim(matrix, col_offset, own_width, matrix.ndim - 1)

    whole_rows = lax.all_gather(
        residual_channel.reshape(row_count, own_width), "tp", axis=1, tiled=True
    )
    current = whole_rows
    for block_index_number in range(LAYERS):
        widened = whole_rows.astype(jnp.float32)
        inv_rms = lax.rsqrt(jnp.mean(widened * widened, axis=-1, keepdims=True) + EPS)
        hidden = (widened * inv_rms * prior_block_multiplier[block_index_number]).astype(
            jnp.bfloat16
        )
        weights = (
            probe_map_matrix[block_index_number],
            lookup_map_matrix[block_index_number],
            content_map_matrix[block_index_number],
            emission_valve_matrix[block_index_number],
            lax.dynamic_slice_in_dim(
                forgetting_map_matrix[block_index_number], head_offset, head_count, 1
            ),
            lax.dynamic_slice_in_dim(
                insertion_rate_matrix[block_index_number], head_offset, head_count, 1
            ),
        )
        mapped_token_vectors = project(hidden, weights)
        mixed_out = mix_layer(mapped_token_vectors, block_index_number)
        if block_index_number < LAYERS - 1:
            gathered = lax.all_gather(mixed_out, "tp", axis=1, tiled=True)
            whole_rows = post_residual(
                widened, gathered, post_mixing_multiplier[block_index_number], True
            )
        else:
            current = post_residual(
                own_cols(widened),
                mixed_out,
                own_cols(post_mixing_multiplier[block_index_number]),
                False,
            )
    return (
        current.reshape(batch_total, generation_round_total, own_width),
        jnp.stack(new_states, axis=0),
    )


def local_two_heads(
    residual_channel,
    prior_block_multiplier,
    probe_map_matrix,
    lookup_map_matrix,
    content_map_matrix,
    emission_valve_matrix,
    forgetting_map_matrix,
    insertion_rate_matrix,
    forgetting_magnitude_exponent,
    channel_forgetting_offset,
    surplus_forgetting_amounts,
    readout_rescale_multiplier,
    emission_map_matrix,
    post_mixing_multiplier,
    recurrent_matrices,
):
    batch_total, steps, own_width = residual_channel.shape
    layers, _, head_count, state_size = recurrent_matrices.shape
    row_count = batch_total * steps
    col_offset = lax.axis_index("tp") * own_width
    head_offset = lax.axis_index("tp") * head_count

    def own_cols(matrix):
        return lax.dynamic_slice_in_dim(matrix, col_offset, own_width, matrix.ndim - 1)

    whole_rows = lax.all_gather(
        residual_channel.reshape(row_count, own_width), "tp", axis=1, tiled=True
    )
    constants = mixer_constants(head_count)
    groups = state_size // LANES
    states = (
        recurrent_matrices.reshape(layers, batch_total, head_count, groups, LANES)
        .transpose(0, 1, 3, 2, 4)
        .reshape(layers, batch_total, groups * head_count, LANES)
    )
    rates = [
        lax.dynamic_slice_in_dim(matrix, head_offset, head_count, 2)
        for matrix in (forgetting_map_matrix, insertion_rate_matrix)
    ]
    filler = jnp.zeros(rates[0].shape[:2] + (LANES - 2 * head_count,), jnp.bfloat16)
    weights = [
        jnp.concatenate(
            [
                matrix[layer]
                for matrix in (
                    probe_map_matrix,
                    lookup_map_matrix,
                    content_map_matrix,
                    emission_valve_matrix,
                    rates[0],
                    rates[1],
                    filler,
                )
            ],
            axis=1,
        )
        for layer in range(layers)
    ]
    surplus = jnp.repeat(
        surplus_forgetting_amounts.reshape(layers, row_count, head_count), HEAD_DIM, axis=2
    )
    vectors = jnp.stack(
        [
            jnp.repeat(-jnp.exp(forgetting_magnitude_exponent), HEAD_DIM, axis=1),
            jnp.repeat(channel_forgetting_offset, HEAD_DIM, axis=1),
            readout_rescale_multiplier,
        ],
        axis=1,
    )
    earlier = None
    current = None
    for layer in range(layers):
        widened = whole_rows.astype(jnp.float32)
        inv_rms = lax.rsqrt(jnp.mean(widened * widened, axis=-1, keepdims=True) + EPS)
        hidden = (widened * inv_rms * prior_block_multiplier[layer]).astype(jnp.bfloat16)
        proj = jnp.dot(hidden, weights[layer], preferred_element_type=jnp.float32).astype(
            jnp.bfloat16
        )
        readout, earlier = mixer(
            proj, surplus[layer], vectors[layer], constants, states, layer, earlier
        )
        mixed_out = out_project(readout, emission_map_matrix[layer])
        if layer < layers - 1:
            gathered = lax.all_gather(mixed_out, "tp", axis=1, tiled=True)
            whole_rows = post_residual(widened, gathered, post_mixing_multiplier[layer], True)
        else:
            current = post_residual(
                own_cols(whole_rows).astype(jnp.float32),
                mixed_out,
                own_cols(post_mixing_multiplier[layer]),
                False,
            )
    new_memory = (
        earlier.reshape(layers, batch_total, groups, head_count, LANES)
        .transpose(0, 1, 3, 2, 4)
        .reshape(recurrent_matrices.shape)
    )
    return current.reshape(batch_total, steps, own_width), new_memory


def local_any(*arrays):
    residual_channel, recurrent_matrices = arrays[0], arrays[-1]
    two_heads = recurrent_matrices.shape[2] * HEAD_DIM == LANES and residual_channel.shape[1] == 8
    return (local_two_heads if two_heads else local)(*arrays)


def solution(mesh):
    return jax.shard_map(
        local_any,
        mesh=mesh,
        in_specs=(
            P("grp", None, "tp"),
            P(),
            P(None, None, "tp"),
            P(None, None, "tp"),
            P(None, None, "tp"),
            P(None, None, "tp"),
            P(),
            P(),
            P(None, "tp"),
            P(None, "tp"),
            P(None, "grp", None, "tp"),
            P(None, "tp"),
            P(None, None, "tp"),
            P(),
            P(None, "grp", "tp", None),
        ),
        out_specs=(P("grp", None, "tp"), P(None, "grp", "tp", None)),
        check_vma=False,
    )
```

```python
import jax
import jax.numpy as jnp
from jax import lax
from jax.experimental import pallas as pl
from jax.experimental.pallas import tpu as pltpu
from jax.sharding import PartitionSpec as P

D = 4096
HEAD_DIM = 64
LAYERS = 2


EPS = 1e-06
HIGH = lax.Precision.HIGHEST


def solve_lower(a_mat, right_side):
    length = right_side.shape[-2]
    solved_rows = []
    for row_at in range(length):
        current_row = right_side[..., row_at, :]
        for col_at in range(row_at):
            current_row = current_row - a_mat[..., row_at, col_at][..., None] * solved_rows[col_at]
        solved_rows.append(current_row)
    return jnp.stack(solved_rows, axis=-2)


def delta_block(queries, key_rows, values, forgetting_exponent_amount, strength, matrix_state):
    length = queries.shape[2]
    causal = jnp.tril(jnp.ones((length, length), bool))
    strict = jnp.tril(jnp.ones((length, length), bool), -1)
    cumulative = jnp.cumsum(forgetting_exponent_amount, axis=-1)
    decay_mat = jnp.where(
        causal,
        jnp.exp(jnp.where(causal, cumulative[..., :, None] - cumulative[..., None, :], 0.0)),
        0.0,
    )
    key_gram = jnp.einsum("bhtd,bhsd->bhts", key_rows, key_rows, precision=HIGH)
    a_mat = jnp.where(strict, strength[..., :, None] * decay_mat * key_gram, 0.0)
    right_side = jnp.concatenate(
        [strength[..., None] * values, (strength * jnp.exp(cumulative))[..., None] * key_rows],
        axis=-1,
    )
    solved = solve_lower(a_mat, right_side)
    width_v = values.shape[-1]
    update = solved[..., :width_v] - jnp.einsum(
        "bhtk,bhkv->bhtv", solved[..., width_v:], matrix_state, precision=HIGH
    )
    scores = jnp.einsum("bhtd,bhsd->bhts", queries, key_rows, precision=HIGH) * decay_mat
    output = jnp.exp(cumulative)[..., None] * jnp.einsum(
        "bhtk,bhkv->bhtv", queries, matrix_state, precision=HIGH
    )
    output = output + jnp.einsum("bhts,bhsv->bhtv", scores, update, precision=HIGH)
    final_log = cumulative[..., -1:]
    revised_memory_matrix = jnp.exp(final_log)[..., None] * matrix_state + jnp.einsum(
        "bhsk,bhsv->bhkv",
        key_rows * jnp.exp(final_log - cumulative)[..., None],
        update,
        precision=HIGH,
    )
    return (output, revised_memory_matrix)


def unit_rows(matrix):
    return matrix * lax.rsqrt(jnp.sum(matrix * matrix, axis=-1, keepdims=True) + EPS)


def token_blender(
    mapped_token_vectors,
    magnitude_exponent,
    offset_terms_array,
    surplus_forgetting_exponent,
    multiplier_terms_array,
    incoming_memory_matrix,
    batch_total,
    generation_round_total,
):
    rounded = [
        lax.optimization_barrier(part_sum.astype(jnp.bfloat16)).astype(jnp.float32)
        for part_sum in mapped_token_vectors
    ]
    queries, keys_raw, values_raw, gate_raw, decay_pre, strength_pre = rounded
    head_count = incoming_memory_matrix.shape[1]

    def to_heads(matrix):
        return matrix.reshape(batch_total, generation_round_total, head_count, HEAD_DIM).transpose(
            0, 2, 1, 3
        )

    def per_head(matrix):
        return matrix.reshape(batch_total, generation_round_total, head_count).transpose(0, 2, 1)

    queries = unit_rows(jax.nn.silu(to_heads(queries))) * HEAD_DIM ** (-0.5)
    key_rows = unit_rows(jax.nn.silu(to_heads(keys_raw)))
    values = jax.nn.silu(to_heads(values_raw))
    forgetting_exponent_amount = -jnp.exp(magnitude_exponent)[None, :, None] * jax.nn.softplus(
        per_head(decay_pre) + offset_terms_array[None, :, None]
    )
    forgetting_exponent_amount = forgetting_exponent_amount + surplus_forgetting_exponent.transpose(
        0, 2, 1
    )
    strength = jax.nn.sigmoid(per_head(strength_pre))
    matrix_state = incoming_memory_matrix.reshape(batch_total, head_count, HEAD_DIM, HEAD_DIM)
    output, revised_memory_matrix = delta_block(
        queries, key_rows, values, forgetting_exponent_amount, strength, matrix_state
    )
    normed = output * lax.rsqrt(jnp.mean(output * output, axis=-1, keepdims=True) + EPS)
    normed = (
        normed
        * multiplier_terms_array.reshape(head_count, HEAD_DIM)[None, :, None, :]
        * jax.nn.silu(to_heads(gate_raw))
    )
    blended_token_vectors = (
        normed.transpose(0, 2, 1, 3)
        .reshape(batch_total * generation_round_total, head_count * HEAD_DIM)
        .astype(jnp.bfloat16)
    )
    return (
        blended_token_vectors,
        revised_memory_matrix.reshape(batch_total, head_count, HEAD_DIM * HEAD_DIM),
    )


LANES = 128


def bf16_dot(left, right):
    return jnp.dot(left, right, preferred_element_type=jnp.float32)


def head_sums(squares, ones):
    high = squares.astype(jnp.bfloat16)
    low = (squares - high.astype(jnp.float32)).astype(jnp.bfloat16)
    return bf16_dot(high, ones) + bf16_dot(low, ones)


def mixer_kernel(
    proj_ref, surplus_ref, vec_ref, spread_ref, ones_ref, perm_ref, state_ref, *rest
):
    y_ref, new_ref, qk_ref, x_ref, kd_ref, u_ref, qs_ref, dec_ref = rest[-8:]
    rows = proj_ref.shape[0]
    seqs, steps = qk_ref.shape[1], qk_ref.shape[2]
    f32, bf16 = jnp.float32, jnp.bfloat16
    ones = ones_ref[...]
    perm = perm_ref[...]

    def cols(at):
        return proj_ref[:, at * LANES : (at + 1) * LANES].astype(f32)

    def tokens(matrix):
        return matrix.reshape(seqs, steps, LANES)

    queries = jax.nn.silu(cols(0))
    keys = jax.nn.silu(cols(1))
    sums = head_sums(jnp.concatenate([queries * queries, keys * keys], axis=1), ones)
    queries = tokens(queries * lax.rsqrt(sums[:, :LANES] + EPS) * HEAD_DIM ** (-0.5))
    keys = tokens(keys * lax.rsqrt(sums[:, LANES:] + EPS))
    spread = bf16_dot(proj_ref[:, 4 * LANES : 5 * LANES], spread_ref[...])
    biased = spread[:, :LANES] + vec_ref[1:2, :]
    softplus = jnp.maximum(biased, 0.0) + jnp.log1p(jnp.exp(-jnp.abs(biased)))
    cumulative = tokens(vec_ref[0:1, :] * softplus + surplus_ref[...])
    beta = tokens(jax.nn.sigmoid(spread[:, LANES:]))
    token = lax.broadcasted_iota(jnp.int32, (seqs, steps, LANES), 1)
    shift = 1
    while shift < steps:
        moved = pltpu.roll(cumulative, shift, axis=1)
        cumulative = cumulative + jnp.where(token >= shift, moved, 0.0)
        shift *= 2
    grown = jnp.exp(cumulative)
    solved_u = beta * tokens(jax.nn.silu(cols(2)))
    solved_p = beta * grown * keys
    for at in range(steps):
        causal = token >= at
        gap = jnp.where(causal, cumulative - cumulative[:, at : at + 1, :], 0.0)
        decay = jnp.where(causal, jnp.exp(gap), 0.0)
        key_row = keys[:, at : at + 1, :]
        pair = jnp.concatenate([queries * key_row, keys * key_row], axis=2)
        dots = bf16_dot(pair.reshape(rows, 2 * LANES).astype(bf16), ones)
        qk_ref[at] = tokens(dots[:, :LANES]) * decay
        if at < steps - 1:
            a_col = jnp.where(token > at, beta * decay * tokens(dots[:, LANES:]), 0.0)
            solved_u = solved_u - a_col * solved_u[:, at : at + 1, :]
            solved_p = solved_p - a_col * solved_p[:, at : at + 1, :]
    last = cumulative[:, steps - 1 : steps, :]
    faded = keys * jnp.exp(last - cumulative)

    def permuted(first, second):
        both = jnp.concatenate([first, second], axis=1).reshape(2 * rows, LANES)
        return bf16_dot(both.astype(bf16), perm).astype(bf16).reshape(seqs, 2 * steps, LANES)

    x_ref[...] = permuted(queries, solved_p)
    kd_ref[...] = permuted(faded, faded)
    u_ref[...] = solved_u
    dec_ref[...] = jnp.broadcast_to(jnp.exp(last), (seqs, steps, LANES))

    state_rows = state_ref.shape[2]
    even = lax.broadcasted_iota(jnp.int32, (state_rows, LANES), 0) % 2 == 0
    left = lax.broadcasted_iota(jnp.int32, (state_rows, LANES), 1) < HEAD_DIM
    kept = even == left

    def one_sequence(at, carry):
        state = state_ref[0, at]
        turned = pltpu.roll(state, HEAD_DIM, axis=1)
        upper = jnp.where(kept, jnp.where(even, state, turned), 0.0)
        lower = jnp.where(kept, jnp.where(even, turned, state), 0.0)
        wide = jnp.concatenate([upper, lower], axis=0).astype(bf16)
        read = bf16_dot(x_ref[at], wide)
        qs_ref[at] = read[:steps]
        update = u_ref[at] - read[steps:]
        u_ref[at] = update
        high = update.astype(bf16).astype(f32)
        split = jnp.concatenate([high, update - high], axis=0).astype(bf16)
        grow = lax.dot_general(
            kd_ref[at], split, (((0,), (0,)), ((), ())), preferred_element_type=f32
        )
        grow_0, grow_1 = grow[:state_rows], grow[state_rows:]
        crossed = pltpu.roll(jnp.where(even, grow_1, grow_0), HEAD_DIM, axis=1)
        added = jnp.where(kept, jnp.where(even, grow_0, grow_1), crossed)
        fade = dec_ref[at]
        fade_turned = pltpu.roll(fade, HEAD_DIM, axis=1)
        copies = state_rows // steps
        factor = jnp.where(
            kept,
            jnp.concatenate([fade] * copies, axis=0),
            jnp.concatenate([fade_turned] * copies, axis=0),
        )
        new_ref[0, at] = factor * state + added
        return carry

    lax.fori_loop(0, seqs, one_sequence, 0, unroll=4)
    update = u_ref[...]
    output = grown * qs_ref[...]
    for at in range(steps):
        output = output + qk_ref[at] * update[:, at : at + 1, :]
    output = output.reshape(rows, LANES)
    squares = head_sums(output * output, ones[:LANES, :LANES])
    output = output * lax.rsqrt(squares * (1.0 / HEAD_DIM) + EPS)
    y_ref[...] = (output * vec_ref[2:3, :] * jax.nn.silu(cols(3))).astype(bf16)


def mixer_constants(head_count):
    row = jnp.arange(2 * LANES)[:, None]
    col = jnp.arange(2 * LANES)[None, :]
    ones = (row // HEAD_DIM == col // HEAD_DIM).astype(jnp.bfloat16)
    spread = (row[:LANES] == col // HEAD_DIM).astype(jnp.bfloat16)
    head, channel = row[:LANES] // HEAD_DIM, row[:LANES] % HEAD_DIM
    target = (channel % 2) * HEAD_DIM + (channel // 2) * head_count + head
    perm = (target == col[:, :LANES]).astype(jnp.bfloat16)
    return spread, ones, perm


def mixer(proj, surplus, vectors, constants, states, layer, earlier):
    rows = proj.shape[0]
    layers, all_seqs, state_rows, _ = states.shape
    seqs_here = all_seqs
    steps = rows // seqs_here
    block = next(size for size in (32, 16, 8, 4, 2, 1) if seqs_here % size == 0)
    token_rows = block * steps
    spread, ones, perm = constants

    def whole(array):
        return pl.BlockSpec(array.shape, lambda i: (0,) * array.ndim)

    in_specs = [
        pl.BlockSpec((token_rows, proj.shape[1]), lambda i: (i, 0)),
        pl.BlockSpec((token_rows, LANES), lambda i: (i, 0)),
        whole(vectors),
        whole(spread),
        whole(ones),
        whole(perm),
        pl.BlockSpec((1, block, state_rows, LANES), lambda i: (layer, i, 0, 0)),
    ]
    operands = [proj, surplus, vectors, spread, ones, perm, states]
    aliases = {}
    if earlier is not None:
        in_specs.append(pl.BlockSpec(memory_space=pl.ANY))
        operands.append(earlier)
        aliases = {len(operands) - 1: 1}
    tile = (block, steps, LANES)
    return pl.pallas_call(
        mixer_kernel,
        grid=(seqs_here // block,),
        in_specs=in_specs,
        out_specs=[
            pl.BlockSpec((token_rows, LANES), lambda i: (i, 0)),
            pl.BlockSpec((1, block, state_rows, LANES), lambda i: (layer, i, 0, 0)),
        ],
        out_shape=[
            jax.ShapeDtypeStruct((rows, LANES), jnp.bfloat16),
            jax.ShapeDtypeStruct(states.shape, jnp.float32),
        ],
        scratch_shapes=[
            pltpu.VMEM((steps,) + tile, jnp.float32),
            pltpu.VMEM((block, 2 * steps, LANES), jnp.bfloat16),
            pltpu.VMEM((block, 2 * steps, LANES), jnp.bfloat16),
            pltpu.VMEM(tile, jnp.float32),
            pltpu.VMEM(tile, jnp.float32),
            pltpu.VMEM(tile, jnp.float32),
        ],
        input_output_aliases=aliases,
        cost_estimate=pl.CostEstimate(
            flops=rows * 20 * 2 * LANES * 2 * LANES,
            bytes_accessed=2 * all_seqs * state_rows * LANES * 4,
            transcendentals=rows * LANES * 12,
        ),
        name="mixer",
    )(*operands)


def project(portion, weights):
    return tuple(
        (jnp.dot(portion, weight, preferred_element_type=jnp.float32) for weight in weights)
    )


def out_project(blended_token_vectors, weight_rows):
    return jnp.dot(
        lax.all_gather(blended_token_vectors, "tp", axis=1, tiled=True),
        weight_rows,
        preferred_element_type=jnp.float32,
    ).astype(jnp.bfloat16)


def post_residual(widened, mixed_out, multiplier_terms_array, complete):
    mixed_wide = lax.optimization_barrier(mixed_out).astype(jnp.float32)
    squares = jnp.sum(mixed_wide * mixed_wide, axis=-1)
    if not complete:
        squares = lax.psum(squares, "tp")
    post_rms = lax.rsqrt(squares / D + EPS)[:, None]
    return lax.optimization_barrier(
        (widened + mixed_wide * post_rms * multiplier_terms_array).astype(jnp.bfloat16)
    )


def local(
    residual_channel,
    prior_block_multiplier,
    probe_map_matrix,
    lookup_map_matrix,
    content_map_matrix,
    emission_valve_matrix,
    forgetting_map_matrix,
    insertion_rate_matrix,
    forgetting_magnitude_exponent,
    channel_forgetting_offset,
    surplus_forgetting_amounts,
    readout_rescale_multiplier,
    emission_map_matrix,
    post_mixing_multiplier,
    recurrent_matrices,
):
    batch_total, generation_round_total, own_width = residual_channel.shape
    head_count = recurrent_matrices.shape[2]
    row_count = batch_total * generation_round_total
    col_offset = lax.axis_index("tp") * own_width
    head_offset = lax.axis_index("tp") * head_count
    new_states = []

    def mix_layer(mapped_token_vectors, block_index_number):
        blended_token_vectors, revised_memory_matrix = token_blender(
            mapped_token_vectors,
            forgetting_magnitude_exponent[block_index_number],
            channel_forgetting_offset[block_index_number],
            surplus_forgetting_amounts[block_index_number],
            readout_rescale_multiplier[block_index_number],
            recurrent_matrices[block_index_number],
            batch_total,
            generation_round_total,
        )
        new_states.append(revised_memory_matrix)
        return out_project(blended_token_vectors, emission_map_matrix[block_index_number])

    def own_cols(matrix):
        return lax.dynamic_slice_in_dim(matrix, col_offset, own_width, matrix.ndim - 1)

    whole_rows = lax.all_gather(
        residual_channel.reshape(row_count, own_width), "tp", axis=1, tiled=True
    )
    current = whole_rows
    for block_index_number in range(LAYERS):
        widened = whole_rows.astype(jnp.float32)
        inv_rms = lax.rsqrt(jnp.mean(widened * widened, axis=-1, keepdims=True) + EPS)
        hidden = (widened * inv_rms * prior_block_multiplier[block_index_number]).astype(
            jnp.bfloat16
        )
        weights = (
            probe_map_matrix[block_index_number],
            lookup_map_matrix[block_index_number],
            content_map_matrix[block_index_number],
            emission_valve_matrix[block_index_number],
            lax.dynamic_slice_in_dim(
                forgetting_map_matrix[block_index_number], head_offset, head_count, 1
            ),
            lax.dynamic_slice_in_dim(
                insertion_rate_matrix[block_index_number], head_offset, head_count, 1
            ),
        )
        mapped_token_vectors = project(hidden, weights)
        mixed_out = mix_layer(mapped_token_vectors, block_index_number)
        if block_index_number < LAYERS - 1:
            gathered = lax.all_gather(mixed_out, "tp", axis=1, tiled=True)
            whole_rows = post_residual(
                widened, gathered, post_mixing_multiplier[block_index_number], True
            )
        else:
            current = post_residual(
                own_cols(widened),
                mixed_out,
                own_cols(post_mixing_multiplier[block_index_number]),
                False,
            )
    return (
        current.reshape(batch_total, generation_round_total, own_width),
        jnp.stack(new_states, axis=0),
    )


PARTS = 2


def gather_kernel(count, src_ref, out_ref, right_sem, left_sem, over_sem, twin_sem, land_sem, own_sem):
    me = lax.axis_index("tp")
    depth = count // 4
    core, row, line = lax.rem(me, 2), lax.rem(me // 2, 2), me // 4
    over, twin = me + 2 - 4 * row, me + 1 - 2 * core
    width = src_ref.shape[1]
    part_rows = src_ref.shape[0] // PARTS
    has_left, has_right = line > 0, line < depth - 1
    barrier = pltpu.get_barrier_semaphore()

    def greet(device):
        pl.semaphore_signal(
            barrier, inc=1, device_id={"tp": device}, device_id_type=pl.DeviceIdType.MESH
        )

    greet(over)
    greet(twin)

    greet(lax.rem(me + 4, count))
    greet(lax.rem(me + count - 4, count))
    pl.semaphore_wait(barrier, 4)

    def spot(origin, part):
        return out_ref.at[
            pl.ds(part * part_rows, part_rows), pl.ds(pl.multiple_of(origin * width, 128), width)
        ]

    def transfer(origin, part, device, send_sem, own):
        source = src_ref.at[pl.ds(part * part_rows, part_rows), :] if own else spot(origin, part)
        return pltpu.make_async_remote_copy(
            src_ref=source,
            dst_ref=spot(origin, part),
            send_sem=send_sem,
            recv_sem=land_sem.at[origin, part],
            device_id={"tp": device},
            device_id_type=pl.DeviceIdType.MESH,
        )

    ending = []

    def send(origin, part, device, send_sem, when, own=False):
        @pl.when(when)
        def _():
            transfer(origin, part, device, send_sem, own).start()

        def finish():
            @pl.when(when)
            def _():
                transfer(origin, part, device, send_sem, own).wait_send()

        ending.append(finish)

    def arrived(origin, part, when):
        @pl.when(when)
        def _():
            transfer(origin, part, twin, twin_sem.at[0, 0], False).wait_recv()

    always = line >= 0
    own_copies = []
    for part in range(PARTS):
        send(me, part, me + 4, right_sem.at[0, part], has_right, True)
        send(me, part, me - 4, left_sem.at[0, part], has_left, True)
        send(me, part, over, over_sem.at[0, part], always, True)
        send(me, part, twin, twin_sem.at[0, part], always, True)
        copy = pltpu.make_async_copy(
            src_ref.at[pl.ds(part * part_rows, part_rows), :], spot(me, part), own_sem.at[part]
        )
        copy.start()
        own_copies.append(copy)

    def crossing(hop):
        for part in range(PARTS):
            if hop == 0:
                arrived(over, part, always)
                send(over, part, twin, twin_sem.at[1, part], always)
            else:
                arrived(over - 4 * hop, part, line >= hop)
                send(over - 4 * hop, part, twin, twin_sem.at[4 * hop + 2, part], line >= hop)
                ahead = line + hop < depth
                arrived(over + 4 * hop, part, ahead)
                send(over + 4 * hop, part, twin, twin_sem.at[4 * hop + 3, part], ahead)

    for hop in range(1, depth):
        for part in range(PARTS):
            behind, ahead = line >= hop, line + hop < depth
            origin = me - 4 * hop
            arrived(origin, part, behind)
            if hop < depth - 1:
                send(origin, part, me + 4, right_sem.at[hop, part], behind & has_right)
            send(origin, part, over, over_sem.at[2 * hop, part], behind)
            send(origin, part, twin, twin_sem.at[4 * hop, part], behind)
            origin = me + 4 * hop
            arrived(origin, part, ahead)
            if hop < depth - 1:
                send(origin, part, me - 4, left_sem.at[hop, part], ahead & has_left)
            send(origin, part, over, over_sem.at[2 * hop + 1, part], ahead)
            send(origin, part, twin, twin_sem.at[4 * hop + 1, part], ahead)
        crossing(hop - 1)
    crossing(depth - 1)
    for place in range(count // 2):
        for part in range(PARTS):
            arrived(2 * place + 1 - core, part, always)
    for finish in ending:
        finish()
    for copy in own_copies:
        copy.wait()


def gather_columns(block, count, collective):
    rows, width = block.shape
    depth = count // 4
    dma = pltpu.SemaphoreType.DMA
    return pl.pallas_call(
        lambda *refs: gather_kernel(count, *refs),
        out_shape=jax.ShapeDtypeStruct((rows, count * width), block.dtype),
        in_specs=[pl.BlockSpec(memory_space=pltpu.VMEM)],
        out_specs=pl.BlockSpec(memory_space=pl.ANY),
        scratch_shapes=[
            dma((depth, PARTS)),
            dma((depth, PARTS)),
            dma((2 * depth, PARTS)),
            dma((4 * depth, PARTS)),
            dma((count, PARTS)),
            dma((PARTS,)),
        ],
        compiler_params=pltpu.CompilerParams(collective_id=collective, has_side_effects=True),
        cost_estimate=pl.CostEstimate(
            flops=0, bytes_accessed=count * rows * width * 2, transcendentals=0
        ),
        name="gather_columns",
    )(block)


def total_kernel(count, src_ref, out_ref, held_ref, send_sem, land_sem):
    me = lax.axis_index("tp")
    barrier = pltpu.get_barrier_semaphore()
    for step in range(1, count):
        pl.semaphore_signal(
            barrier,
            inc=1,
            device_id={"tp": lax.rem(me + step, count)},
            device_id_type=pl.DeviceIdType.MESH,
        )
    pl.semaphore_wait(barrier, count - 1)
    copies = []
    for step in range(1, count):
        copies.append(
            pltpu.make_async_remote_copy(
                src_ref=src_ref,
                dst_ref=held_ref.at[step],
                send_sem=send_sem.at[step],
                recv_sem=land_sem.at[step],
                device_id={"tp": lax.rem(me + step, count)},
                device_id_type=pl.DeviceIdType.MESH,
            )
        )
        copies[-1].start()
    total = src_ref[...]
    for step, copy in enumerate(copies):
        copy.wait_recv()
        total = total + held_ref[step + 1]
    out_ref[...] = total
    for copy in copies:
        copy.wait_send()


def total_over(sums, count, collective):
    tile = (sums.shape[0] // LANES, LANES)
    dma = pltpu.SemaphoreType.DMA
    total = pl.pallas_call(
        lambda *refs: total_kernel(count, *refs),
        out_shape=jax.ShapeDtypeStruct(tile, sums.dtype),
        in_specs=[pl.BlockSpec(memory_space=pltpu.VMEM)],
        out_specs=pl.BlockSpec(memory_space=pltpu.VMEM),
        scratch_shapes=[pltpu.VMEM((count,) + tile, sums.dtype), dma((count,)), dma((count,))],
        compiler_params=pltpu.CompilerParams(collective_id=collective, has_side_effects=True),
        name="total_over",
    )(sums.reshape(tile))
    return total.reshape(sums.shape)


def local_two_heads(
    residual_channel,
    prior_block_multiplier,
    probe_map_matrix,
    lookup_map_matrix,
    content_map_matrix,
    emission_valve_matrix,
    forgetting_map_matrix,
    insertion_rate_matrix,
    forgetting_magnitude_exponent,
    channel_forgetting_offset,
    surplus_forgetting_amounts,
    readout_rescale_multiplier,
    emission_map_matrix,
    post_mixing_multiplier,
    recurrent_matrices,
):
    batch_total, steps, own_width = residual_channel.shape
    layers, _, head_count, state_size = recurrent_matrices.shape
    row_count = batch_total * steps
    col_offset = lax.axis_index("tp") * own_width
    head_offset = lax.axis_index("tp") * head_count
    device_count = lax.axis_size("tp")

    def own_cols(matrix):
        return lax.dynamic_slice_in_dim(matrix, col_offset, own_width, matrix.ndim - 1)

    whole_rows = lax.all_gather(
        residual_channel.reshape(row_count, own_width), "tp", axis=1, tiled=True
    )
    constants = mixer_constants(head_count)
    groups = state_size // LANES
    states = (
        recurrent_matrices.reshape(layers, batch_total, head_count, groups, LANES)
        .transpose(0, 1, 3, 2, 4)
        .reshape(layers, batch_total, groups * head_count, LANES)
    )
    rates = [
        lax.dynamic_slice_in_dim(matrix, head_offset, head_count, 2)
        for matrix in (forgetting_map_matrix, insertion_rate_matrix)
    ]
    filler = jnp.zeros(rates[0].shape[:2] + (LANES - 2 * head_count,), jnp.bfloat16)
    weights = [
        jnp.concatenate(
            [
                matrix[layer]
                for matrix in (
                    probe_map_matrix,
                    lookup_map_matrix,
                    content_map_matrix,
                    emission_valve_matrix,
                    rates[0],
                    rates[1],
                    filler,
                )
            ],
            axis=1,
        )
        for layer in range(layers)
    ]
    surplus = jnp.repeat(
        surplus_forgetting_amounts.reshape(layers, row_count, head_count), HEAD_DIM, axis=2
    )
    vectors = jnp.stack(
        [
            jnp.repeat(-jnp.exp(forgetting_magnitude_exponent), HEAD_DIM, axis=1),
            jnp.repeat(channel_forgetting_offset, HEAD_DIM, axis=1),
            readout_rescale_multiplier,
        ],
        axis=1,
    )
    earlier = None
    current = None
    for layer in range(layers):
        widened = whole_rows.astype(jnp.float32)
        inv_rms = lax.rsqrt(jnp.mean(widened * widened, axis=-1, keepdims=True) + EPS)
        hidden = (widened * inv_rms * prior_block_multiplier[layer]).astype(jnp.bfloat16)
        proj = jnp.dot(hidden, weights[layer], preferred_element_type=jnp.float32).astype(
            jnp.bfloat16
        )
        readout, earlier = mixer(
            proj, surplus[layer], vectors[layer], constants, states, layer, earlier
        )
        spread_out = gather_columns(readout, device_count, 2 * layer + 1)
        mixed_out = jnp.dot(
            spread_out, emission_map_matrix[layer], preferred_element_type=jnp.float32
        ).astype(jnp.bfloat16)
        if layer < layers - 1:
            gathered = gather_columns(mixed_out, device_count, 2 * layer + 2)
            whole_rows = post_residual(widened, gathered, post_mixing_multiplier[layer], True)
        else:
            mixed_wide = lax.optimization_barrier(mixed_out).astype(jnp.float32)
            squares = total_over(
                jnp.sum(mixed_wide * mixed_wide, axis=-1), device_count, 2 * layer + 2
            )
            post_rms = lax.rsqrt(squares / D + EPS)[:, None]
            current = (
                own_cols(whole_rows).astype(jnp.float32)
                + mixed_wide * post_rms * own_cols(post_mixing_multiplier[layer])
            ).astype(jnp.bfloat16)
    new_memory = (
        earlier.reshape(layers, batch_total, groups, head_count, LANES)
        .transpose(0, 1, 3, 2, 4)
        .reshape(recurrent_matrices.shape)
    )
    return current.reshape(batch_total, steps, own_width), new_memory


def local_any(*arrays):
    residual_channel, recurrent_matrices = arrays[0], arrays[-1]
    two_heads = (
        recurrent_matrices.shape[2] * HEAD_DIM == LANES
        and residual_channel.shape[1] == 8
        and residual_channel.shape[0] % 16 == 0
        and residual_channel.shape[2] % LANES == 0
        and lax.axis_size("tp") % 4 == 0
        and lax.axis_size("tp") > 4
    )
    return (local_two_heads if two_heads else local)(*arrays)


def solution(mesh):
    return jax.shard_map(
        local_any,
        mesh=mesh,
        in_specs=(
            P("grp", None, "tp"),
            P(),
            P(None, None, "tp"),
            P(None, None, "tp"),
            P(None, None, "tp"),
            P(None, None, "tp"),
            P(),
            P(),
            P(None, "tp"),
            P(None, "tp"),
            P(None, "grp", None, "tp"),
            P(None, "tp"),
            P(None, None, "tp"),
            P(),
            P(None, "grp", "tp", None),
        ),
        out_specs=(P("grp", None, "tp"), P(None, "grp", "tp", None)),
        check_vma=False,
    )
```

```python
import jax
import jax.numpy as jnp
from jax import lax
from jax.experimental import pallas as pl
from jax.experimental.pallas import tpu as pltpu
from jax.sharding import PartitionSpec as P

D = 4096
HEAD_DIM = 64
LAYERS = 2


EPS = 1e-06
HIGH = lax.Precision.HIGHEST


def solve_lower(a_mat, right_side):
    length = right_side.shape[-2]
    solved_rows = []
    for row_at in range(length):
        current_row = right_side[..., row_at, :]
        for col_at in range(row_at):
            current_row = current_row - a_mat[..., row_at, col_at][..., None] * solved_rows[col_at]
        solved_rows.append(current_row)
    return jnp.stack(solved_rows, axis=-2)


def delta_block(queries, key_rows, values, forgetting_exponent_amount, strength, matrix_state):
    length = queries.shape[2]
    causal = jnp.tril(jnp.ones((length, length), bool))
    strict = jnp.tril(jnp.ones((length, length), bool), -1)
    cumulative = jnp.cumsum(forgetting_exponent_amount, axis=-1)
    decay_mat = jnp.where(
        causal,
        jnp.exp(jnp.where(causal, cumulative[..., :, None] - cumulative[..., None, :], 0.0)),
        0.0,
    )
    key_gram = jnp.einsum("bhtd,bhsd->bhts", key_rows, key_rows, precision=HIGH)
    a_mat = jnp.where(strict, strength[..., :, None] * decay_mat * key_gram, 0.0)
    right_side = jnp.concatenate(
        [strength[..., None] * values, (strength * jnp.exp(cumulative))[..., None] * key_rows],
        axis=-1,
    )
    solved = solve_lower(a_mat, right_side)
    width_v = values.shape[-1]
    update = solved[..., :width_v] - jnp.einsum(
        "bhtk,bhkv->bhtv", solved[..., width_v:], matrix_state, precision=HIGH
    )
    scores = jnp.einsum("bhtd,bhsd->bhts", queries, key_rows, precision=HIGH) * decay_mat
    output = jnp.exp(cumulative)[..., None] * jnp.einsum(
        "bhtk,bhkv->bhtv", queries, matrix_state, precision=HIGH
    )
    output = output + jnp.einsum("bhts,bhsv->bhtv", scores, update, precision=HIGH)
    final_log = cumulative[..., -1:]
    revised_memory_matrix = jnp.exp(final_log)[..., None] * matrix_state + jnp.einsum(
        "bhsk,bhsv->bhkv",
        key_rows * jnp.exp(final_log - cumulative)[..., None],
        update,
        precision=HIGH,
    )
    return (output, revised_memory_matrix)


def unit_rows(matrix):
    return matrix * lax.rsqrt(jnp.sum(matrix * matrix, axis=-1, keepdims=True) + EPS)


def token_blender(
    mapped_token_vectors,
    magnitude_exponent,
    offset_terms_array,
    surplus_forgetting_exponent,
    multiplier_terms_array,
    incoming_memory_matrix,
    batch_total,
    generation_round_total,
):
    rounded = [
        lax.optimization_barrier(part_sum.astype(jnp.bfloat16)).astype(jnp.float32)
        for part_sum in mapped_token_vectors
    ]
    queries, keys_raw, values_raw, gate_raw, decay_pre, strength_pre = rounded
    head_count = incoming_memory_matrix.shape[1]

    def to_heads(matrix):
        return matrix.reshape(batch_total, generation_round_total, head_count, HEAD_DIM).transpose(
            0, 2, 1, 3
        )

    def per_head(matrix):
        return matrix.reshape(batch_total, generation_round_total, head_count).transpose(0, 2, 1)

    queries = unit_rows(jax.nn.silu(to_heads(queries))) * HEAD_DIM ** (-0.5)
    key_rows = unit_rows(jax.nn.silu(to_heads(keys_raw)))
    values = jax.nn.silu(to_heads(values_raw))
    forgetting_exponent_amount = -jnp.exp(magnitude_exponent)[None, :, None] * jax.nn.softplus(
        per_head(decay_pre) + offset_terms_array[None, :, None]
    )
    forgetting_exponent_amount = forgetting_exponent_amount + surplus_forgetting_exponent.transpose(
        0, 2, 1
    )
    strength = jax.nn.sigmoid(per_head(strength_pre))
    matrix_state = incoming_memory_matrix.reshape(batch_total, head_count, HEAD_DIM, HEAD_DIM)
    output, revised_memory_matrix = delta_block(
        queries, key_rows, values, forgetting_exponent_amount, strength, matrix_state
    )
    normed = output * lax.rsqrt(jnp.mean(output * output, axis=-1, keepdims=True) + EPS)
    normed = (
        normed
        * multiplier_terms_array.reshape(head_count, HEAD_DIM)[None, :, None, :]
        * jax.nn.silu(to_heads(gate_raw))
    )
    blended_token_vectors = (
        normed.transpose(0, 2, 1, 3)
        .reshape(batch_total * generation_round_total, head_count * HEAD_DIM)
        .astype(jnp.bfloat16)
    )
    return (
        blended_token_vectors,
        revised_memory_matrix.reshape(batch_total, head_count, HEAD_DIM * HEAD_DIM),
    )


LANES = 128


def bf16_dot(left, right):
    return jnp.dot(left, right, preferred_element_type=jnp.float32)


def head_sums(squares, ones):
    high = squares.astype(jnp.bfloat16)
    low = (squares - high.astype(jnp.float32)).astype(jnp.bfloat16)
    return bf16_dot(high, ones) + bf16_dot(low, ones)


def mixer_kernel(
    proj_ref, surplus_ref, vec_ref, spread_ref, ones_ref, perm_ref, state_ref, *rest
):
    y_ref, new_ref, qk_ref, x_ref, kd_ref, u_ref, qs_ref, dec_ref = rest[-8:]
    rows = proj_ref.shape[0]
    seqs, steps = qk_ref.shape[1], qk_ref.shape[2]
    f32, bf16 = jnp.float32, jnp.bfloat16
    ones = ones_ref[...]
    perm = perm_ref[...]

    def cols(at):
        return proj_ref[:, at * LANES : (at + 1) * LANES].astype(f32)

    def tokens(matrix):
        return matrix.reshape(seqs, steps, LANES)

    queries = jax.nn.silu(cols(0))
    keys = jax.nn.silu(cols(1))
    sums = head_sums(jnp.concatenate([queries * queries, keys * keys], axis=1), ones)
    queries = tokens(queries * lax.rsqrt(sums[:, :LANES] + EPS) * HEAD_DIM ** (-0.5))
    keys = tokens(keys * lax.rsqrt(sums[:, LANES:] + EPS))
    spread = bf16_dot(proj_ref[:, 4 * LANES : 5 * LANES], spread_ref[...])
    biased = spread[:, :LANES] + vec_ref[1:2, :]
    softplus = jnp.maximum(biased, 0.0) + jnp.log1p(jnp.exp(-jnp.abs(biased)))
    cumulative = tokens(vec_ref[0:1, :] * softplus + surplus_ref[...])
    beta = tokens(jax.nn.sigmoid(spread[:, LANES:]))
    token = lax.broadcasted_iota(jnp.int32, (seqs, steps, LANES), 1)
    shift = 1
    while shift < steps:
        moved = pltpu.roll(cumulative, shift, axis=1)
        cumulative = cumulative + jnp.where(token >= shift, moved, 0.0)
        shift *= 2
    grown = jnp.exp(cumulative)
    solved_u = beta * tokens(jax.nn.silu(cols(2)))
    solved_p = beta * grown * keys
    for at in range(steps):
        causal = token >= at
        gap = jnp.where(causal, cumulative - cumulative[:, at : at + 1, :], 0.0)
        decay = jnp.where(causal, jnp.exp(gap), 0.0)
        key_row = keys[:, at : at + 1, :]
        pair = jnp.concatenate([queries * key_row, keys * key_row], axis=2)
        dots = bf16_dot(pair.reshape(rows, 2 * LANES).astype(bf16), ones)
        qk_ref[at] = tokens(dots[:, :LANES]) * decay
        if at < steps - 1:
            a_col = jnp.where(token > at, beta * decay * tokens(dots[:, LANES:]), 0.0)
            solved_u = solved_u - a_col * solved_u[:, at : at + 1, :]
            solved_p = solved_p - a_col * solved_p[:, at : at + 1, :]
    last = cumulative[:, steps - 1 : steps, :]
    faded = keys * jnp.exp(last - cumulative)

    def permuted(first, second):
        both = jnp.concatenate([first, second], axis=1).reshape(2 * rows, LANES)
        return bf16_dot(both.astype(bf16), perm).astype(bf16).reshape(seqs, 2 * steps, LANES)

    x_ref[...] = permuted(queries, solved_p)
    kd_ref[...] = permuted(faded, faded)
    u_ref[...] = solved_u
    dec_ref[...] = jnp.broadcast_to(jnp.exp(last), (seqs, steps, LANES))

    state_rows = state_ref.shape[2]
    even = lax.broadcasted_iota(jnp.int32, (state_rows, LANES), 0) % 2 == 0
    left = lax.broadcasted_iota(jnp.int32, (state_rows, LANES), 1) < HEAD_DIM
    kept = even == left

    def one_sequence(at, carry):
        state = state_ref[0, at]
        turned = pltpu.roll(state, HEAD_DIM, axis=1)
        upper = jnp.where(kept, jnp.where(even, state, turned), 0.0)
        lower = jnp.where(kept, jnp.where(even, turned, state), 0.0)
        wide = jnp.concatenate([upper, lower], axis=0).astype(bf16)
        read = bf16_dot(x_ref[at], wide)
        qs_ref[at] = read[:steps]
        update = u_ref[at] - read[steps:]
        u_ref[at] = update
        high = update.astype(bf16).astype(f32)
        split = jnp.concatenate([high, update - high], axis=0).astype(bf16)
        grow = lax.dot_general(
            kd_ref[at], split, (((0,), (0,)), ((), ())), preferred_element_type=f32
        )
        grow_0, grow_1 = grow[:state_rows], grow[state_rows:]
        crossed = pltpu.roll(jnp.where(even, grow_1, grow_0), HEAD_DIM, axis=1)
        added = jnp.where(kept, jnp.where(even, grow_0, grow_1), crossed)
        fade = dec_ref[at]
        fade_turned = pltpu.roll(fade, HEAD_DIM, axis=1)
        copies = state_rows // steps
        factor = jnp.where(
            kept,
            jnp.concatenate([fade] * copies, axis=0),
            jnp.concatenate([fade_turned] * copies, axis=0),
        )
        new_ref[0, at] = factor * state + added
        return carry

    lax.fori_loop(0, seqs, one_sequence, 0, unroll=8)
    update = u_ref[...]
    output = grown * qs_ref[...]
    for at in range(steps):
        output = output + qk_ref[at] * update[:, at : at + 1, :]
    output = output.reshape(rows, LANES)
    squares = head_sums(output * output, ones[:LANES, :LANES])
    output = output * lax.rsqrt(squares * (1.0 / HEAD_DIM) + EPS)
    y_ref[...] = (output * vec_ref[2:3, :] * jax.nn.silu(cols(3))).astype(bf16)


def mixer_constants(head_count):
    row = jnp.arange(2 * LANES)[:, None]
    col = jnp.arange(2 * LANES)[None, :]
    ones = (row // HEAD_DIM == col // HEAD_DIM).astype(jnp.bfloat16)
    spread = (row[:LANES] == col // HEAD_DIM).astype(jnp.bfloat16)
    head, channel = row[:LANES] // HEAD_DIM, row[:LANES] % HEAD_DIM
    target = (channel % 2) * HEAD_DIM + (channel // 2) * head_count + head
    perm = (target == col[:, :LANES]).astype(jnp.bfloat16)
    return spread, ones, perm


def mixer(proj, surplus, vectors, constants, states, layer, earlier):
    rows = proj.shape[0]
    layers, all_seqs, state_rows, _ = states.shape
    seqs_here = all_seqs
    steps = rows // seqs_here
    block = next(size for size in (32, 16, 8, 4, 2, 1) if seqs_here % size == 0)
    token_rows = block * steps
    spread, ones, perm = constants

    def whole(array):
        return pl.BlockSpec(array.shape, lambda i: (0,) * array.ndim)

    in_specs = [
        pl.BlockSpec((token_rows, proj.shape[1]), lambda i: (i, 0)),
        pl.BlockSpec((token_rows, LANES), lambda i: (i, 0)),
        whole(vectors),
        whole(spread),
        whole(ones),
        whole(perm),
        pl.BlockSpec((1, block, state_rows, LANES), lambda i: (layer, i, 0, 0)),
    ]
    operands = [proj, surplus, vectors, spread, ones, perm, states]
    aliases = {}
    if earlier is not None:
        in_specs.append(pl.BlockSpec(memory_space=pl.ANY))
        operands.append(earlier)
        aliases = {len(operands) - 1: 1}
    tile = (block, steps, LANES)
    return pl.pallas_call(
        mixer_kernel,
        grid=(seqs_here // block,),
        in_specs=in_specs,
        out_specs=[
            pl.BlockSpec((token_rows, LANES), lambda i: (i, 0)),
            pl.BlockSpec((1, block, state_rows, LANES), lambda i: (layer, i, 0, 0)),
        ],
        out_shape=[
            jax.ShapeDtypeStruct((rows, LANES), jnp.bfloat16),
            jax.ShapeDtypeStruct(states.shape, jnp.float32),
        ],
        scratch_shapes=[
            pltpu.VMEM((steps,) + tile, jnp.float32),
            pltpu.VMEM((block, 2 * steps, LANES), jnp.bfloat16),
            pltpu.VMEM((block, 2 * steps, LANES), jnp.bfloat16),
            pltpu.VMEM(tile, jnp.float32),
            pltpu.VMEM(tile, jnp.float32),
            pltpu.VMEM(tile, jnp.float32),
        ],
        input_output_aliases=aliases,
        cost_estimate=pl.CostEstimate(
            flops=rows * 20 * 2 * LANES * 2 * LANES,
            bytes_accessed=2 * all_seqs * state_rows * LANES * 4,
            transcendentals=rows * LANES * 12,
        ),
        name="mixer",
    )(*operands)


def project(portion, weights):
    return tuple(
        (jnp.dot(portion, weight, preferred_element_type=jnp.float32) for weight in weights)
    )


def out_project(blended_token_vectors, weight_rows):
    return jnp.dot(
        lax.all_gather(blended_token_vectors, "tp", axis=1, tiled=True),
        weight_rows,
        preferred_element_type=jnp.float32,
    ).astype(jnp.bfloat16)


def post_residual(widened, mixed_out, multiplier_terms_array, complete):
    mixed_wide = lax.optimization_barrier(mixed_out).astype(jnp.float32)
    squares = jnp.sum(mixed_wide * mixed_wide, axis=-1)
    if not complete:
        squares = lax.psum(squares, "tp")
    post_rms = lax.rsqrt(squares / D + EPS)[:, None]
    return lax.optimization_barrier(
        (widened + mixed_wide * post_rms * multiplier_terms_array).astype(jnp.bfloat16)
    )


def local(
    residual_channel,
    prior_block_multiplier,
    probe_map_matrix,
    lookup_map_matrix,
    content_map_matrix,
    emission_valve_matrix,
    forgetting_map_matrix,
    insertion_rate_matrix,
    forgetting_magnitude_exponent,
    channel_forgetting_offset,
    surplus_forgetting_amounts,
    readout_rescale_multiplier,
    emission_map_matrix,
    post_mixing_multiplier,
    recurrent_matrices,
):
    batch_total, generation_round_total, own_width = residual_channel.shape
    head_count = recurrent_matrices.shape[2]
    row_count = batch_total * generation_round_total
    col_offset = lax.axis_index("tp") * own_width
    head_offset = lax.axis_index("tp") * head_count
    new_states = []

    def mix_layer(mapped_token_vectors, block_index_number):
        blended_token_vectors, revised_memory_matrix = token_blender(
            mapped_token_vectors,
            forgetting_magnitude_exponent[block_index_number],
            channel_forgetting_offset[block_index_number],
            surplus_forgetting_amounts[block_index_number],
            readout_rescale_multiplier[block_index_number],
            recurrent_matrices[block_index_number],
            batch_total,
            generation_round_total,
        )
        new_states.append(revised_memory_matrix)
        return out_project(blended_token_vectors, emission_map_matrix[block_index_number])

    def own_cols(matrix):
        return lax.dynamic_slice_in_dim(matrix, col_offset, own_width, matrix.ndim - 1)

    whole_rows = lax.all_gather(
        residual_channel.reshape(row_count, own_width), "tp", axis=1, tiled=True
    )
    current = whole_rows
    for block_index_number in range(LAYERS):
        widened = whole_rows.astype(jnp.float32)
        inv_rms = lax.rsqrt(jnp.mean(widened * widened, axis=-1, keepdims=True) + EPS)
        hidden = (widened * inv_rms * prior_block_multiplier[block_index_number]).astype(
            jnp.bfloat16
        )
        weights = (
            probe_map_matrix[block_index_number],
            lookup_map_matrix[block_index_number],
            content_map_matrix[block_index_number],
            emission_valve_matrix[block_index_number],
            lax.dynamic_slice_in_dim(
                forgetting_map_matrix[block_index_number], head_offset, head_count, 1
            ),
            lax.dynamic_slice_in_dim(
                insertion_rate_matrix[block_index_number], head_offset, head_count, 1
            ),
        )
        mapped_token_vectors = project(hidden, weights)
        mixed_out = mix_layer(mapped_token_vectors, block_index_number)
        if block_index_number < LAYERS - 1:
            gathered = lax.all_gather(mixed_out, "tp", axis=1, tiled=True)
            whole_rows = post_residual(
                widened, gathered, post_mixing_multiplier[block_index_number], True
            )
        else:
            current = post_residual(
                own_cols(widened),
                mixed_out,
                own_cols(post_mixing_multiplier[block_index_number]),
                False,
            )
    return (
        current.reshape(batch_total, generation_round_total, own_width),
        jnp.stack(new_states, axis=0),
    )


PARTS = 2


def gather_kernel(count, src_ref, out_ref, right_sem, left_sem, over_sem, twin_sem, land_sem, own_sem):
    me = lax.axis_index("tp")
    depth = count // 4
    core, row, line = lax.rem(me, 2), lax.rem(me // 2, 2), me // 4
    over, twin = me + 2 - 4 * row, me + 1 - 2 * core
    width = src_ref.shape[1]
    part_rows = src_ref.shape[0] // PARTS
    has_left, has_right = line > 0, line < depth - 1
    barrier = pltpu.get_barrier_semaphore()

    def greet(device):
        pl.semaphore_signal(
            barrier, inc=1, device_id={"tp": device}, device_id_type=pl.DeviceIdType.MESH
        )

    greet(over)
    greet(twin)

    greet(lax.rem(me + 4, count))
    greet(lax.rem(me + count - 4, count))
    pl.semaphore_wait(barrier, 4)

    def spot(origin, part):
        return out_ref.at[
            pl.ds(part * part_rows, part_rows), pl.ds(pl.multiple_of(origin * width, 128), width)
        ]

    def transfer(origin, part, device, send_sem, own):
        source = src_ref.at[pl.ds(part * part_rows, part_rows), :] if own else spot(origin, part)
        return pltpu.make_async_remote_copy(
            src_ref=source,
            dst_ref=spot(origin, part),
            send_sem=send_sem,
            recv_sem=land_sem.at[origin, part],
            device_id={"tp": device},
            device_id_type=pl.DeviceIdType.MESH,
        )

    ending = []

    def send(origin, part, device, send_sem, when, own=False):
        @pl.when(when)
        def _():
            transfer(origin, part, device, send_sem, own).start()

        def finish():
            @pl.when(when)
            def _():
                transfer(origin, part, device, send_sem, own).wait_send()

        ending.append(finish)

    def arrived(origin, part, when):
        @pl.when(when)
        def _():
            transfer(origin, part, twin, twin_sem.at[0, 0], False).wait_recv()

    always = line >= 0
    own_copies = []
    for part in range(PARTS):
        send(me, part, me + 4, right_sem.at[0, part], has_right, True)
        send(me, part, me - 4, left_sem.at[0, part], has_left, True)
        send(me, part, over, over_sem.at[0, part], always, True)
        send(me, part, twin, twin_sem.at[0, part], always, True)
        copy = pltpu.make_async_copy(
            src_ref.at[pl.ds(part * part_rows, part_rows), :], spot(me, part), own_sem.at[part]
        )
        copy.start()
        own_copies.append(copy)

    def crossing(hop):
        for part in range(PARTS):
            if hop == 0:
                arrived(over, part, always)
                send(over, part, twin, twin_sem.at[1, part], always)
            else:
                arrived(over - 4 * hop, part, line >= hop)
                send(over - 4 * hop, part, twin, twin_sem.at[4 * hop + 2, part], line >= hop)
                ahead = line + hop < depth
                arrived(over + 4 * hop, part, ahead)
                send(over + 4 * hop, part, twin, twin_sem.at[4 * hop + 3, part], ahead)

    for hop in range(1, depth):
        for part in range(PARTS):
            behind, ahead = line >= hop, line + hop < depth
            origin = me - 4 * hop
            arrived(origin, part, behind)
            if hop < depth - 1:
                send(origin, part, me + 4, right_sem.at[hop, part], behind & has_right)
            send(origin, part, over, over_sem.at[2 * hop, part], behind)
            send(origin, part, twin, twin_sem.at[4 * hop, part], behind)
            origin = me + 4 * hop
            arrived(origin, part, ahead)
            if hop < depth - 1:
                send(origin, part, me - 4, left_sem.at[hop, part], ahead & has_left)
            send(origin, part, over, over_sem.at[2 * hop + 1, part], ahead)
            send(origin, part, twin, twin_sem.at[4 * hop + 1, part], ahead)
        crossing(hop - 1)
    crossing(depth - 1)
    for place in range(count // 2):
        for part in range(PARTS):
            arrived(2 * place + 1 - core, part, always)
    for finish in ending:
        finish()
    for copy in own_copies:
        copy.wait()


def gather_columns(block, count, collective):
    rows, width = block.shape
    depth = count // 4
    dma = pltpu.SemaphoreType.DMA
    return pl.pallas_call(
        lambda *refs: gather_kernel(count, *refs),
        out_shape=jax.ShapeDtypeStruct((rows, count * width), block.dtype),
        in_specs=[pl.BlockSpec(memory_space=pltpu.VMEM)],
        out_specs=pl.BlockSpec(memory_space=pl.ANY),
        scratch_shapes=[
            dma((depth, PARTS)),
            dma((depth, PARTS)),
            dma((2 * depth, PARTS)),
            dma((4 * depth, PARTS)),
            dma((count, PARTS)),
            dma((PARTS,)),
        ],
        compiler_params=pltpu.CompilerParams(collective_id=collective, has_side_effects=True),
        cost_estimate=pl.CostEstimate(
            flops=0, bytes_accessed=count * rows * width * 2, transcendentals=0
        ),
        name="gather_columns",
    )(block)


def total_kernel(count, src_ref, out_ref, held_ref, send_sem, land_sem):
    me = lax.axis_index("tp")
    barrier = pltpu.get_barrier_semaphore()
    for step in range(1, count):
        pl.semaphore_signal(
            barrier,
            inc=1,
            device_id={"tp": lax.rem(me + step, count)},
            device_id_type=pl.DeviceIdType.MESH,
        )
    pl.semaphore_wait(barrier, count - 1)
    copies = []
    for step in range(1, count):
        copies.append(
            pltpu.make_async_remote_copy(
                src_ref=src_ref,
                dst_ref=held_ref.at[step],
                send_sem=send_sem.at[step],
                recv_sem=land_sem.at[step],
                device_id={"tp": lax.rem(me + step, count)},
                device_id_type=pl.DeviceIdType.MESH,
            )
        )
        copies[-1].start()
    total = src_ref[...]
    for step, copy in enumerate(copies):
        copy.wait_recv()
        total = total + held_ref[step + 1]
    out_ref[...] = total
    for copy in copies:
        copy.wait_send()


def total_over(sums, count, collective):
    tile = (sums.shape[0] // LANES, LANES)
    dma = pltpu.SemaphoreType.DMA
    total = pl.pallas_call(
        lambda *refs: total_kernel(count, *refs),
        out_shape=jax.ShapeDtypeStruct(tile, sums.dtype),
        in_specs=[pl.BlockSpec(memory_space=pltpu.VMEM)],
        out_specs=pl.BlockSpec(memory_space=pltpu.VMEM),
        scratch_shapes=[pltpu.VMEM((count,) + tile, sums.dtype), dma((count,)), dma((count,))],
        compiler_params=pltpu.CompilerParams(collective_id=collective, has_side_effects=True),
        name="total_over",
    )(sums.reshape(tile))
    return total.reshape(sums.shape)


def local_two_heads(
    residual_channel,
    prior_block_multiplier,
    probe_map_matrix,
    lookup_map_matrix,
    content_map_matrix,
    emission_valve_matrix,
    forgetting_map_matrix,
    insertion_rate_matrix,
    forgetting_magnitude_exponent,
    channel_forgetting_offset,
    surplus_forgetting_amounts,
    readout_rescale_multiplier,
    emission_map_matrix,
    post_mixing_multiplier,
    recurrent_matrices,
):
    batch_total, steps, own_width = residual_channel.shape
    layers, _, head_count, state_size = recurrent_matrices.shape
    row_count = batch_total * steps
    col_offset = lax.axis_index("tp") * own_width
    head_offset = lax.axis_index("tp") * head_count
    device_count = lax.axis_size("tp")

    def own_cols(matrix):
        return lax.dynamic_slice_in_dim(matrix, col_offset, own_width, matrix.ndim - 1)

    whole_rows = lax.all_gather(
        residual_channel.reshape(row_count, own_width), "tp", axis=1, tiled=True
    )
    constants = mixer_constants(head_count)
    groups = state_size // LANES
    states = (
        recurrent_matrices.reshape(layers, batch_total, head_count, groups, LANES)
        .transpose(0, 1, 3, 2, 4)
        .reshape(layers, batch_total, groups * head_count, LANES)
    )
    rates = [
        lax.dynamic_slice_in_dim(matrix, head_offset, head_count, 2)
        for matrix in (forgetting_map_matrix, insertion_rate_matrix)
    ]
    filler = jnp.zeros(rates[0].shape[:2] + (LANES - 2 * head_count,), jnp.bfloat16)
    weights = [
        jnp.concatenate(
            [
                matrix[layer]
                for matrix in (
                    probe_map_matrix,
                    lookup_map_matrix,
                    content_map_matrix,
                    emission_valve_matrix,
                    rates[0],
                    rates[1],
                    filler,
                )
            ],
            axis=1,
        )
        for layer in range(layers)
    ]
    surplus = jnp.repeat(
        surplus_forgetting_amounts.reshape(layers, row_count, head_count), HEAD_DIM, axis=2
    )
    vectors = jnp.stack(
        [
            jnp.repeat(-jnp.exp(forgetting_magnitude_exponent), HEAD_DIM, axis=1),
            jnp.repeat(channel_forgetting_offset, HEAD_DIM, axis=1),
            readout_rescale_multiplier,
        ],
        axis=1,
    )
    earlier = None
    current = None
    for layer in range(layers):
        widened = whole_rows.astype(jnp.float32)
        inv_rms = lax.rsqrt(jnp.mean(widened * widened, axis=-1, keepdims=True) + EPS)
        hidden = (widened * inv_rms * prior_block_multiplier[layer]).astype(jnp.bfloat16)
        proj = jnp.dot(hidden, weights[layer], preferred_element_type=jnp.float32).astype(
            jnp.bfloat16
        )
        readout, earlier = mixer(
            proj, surplus[layer], vectors[layer], constants, states, layer, earlier
        )
        spread_out = gather_columns(readout, device_count, 2 * layer + 1)
        mixed_out = jnp.dot(
            spread_out, emission_map_matrix[layer], preferred_element_type=jnp.float32
        ).astype(jnp.bfloat16)
        if layer < layers - 1:
            gathered = gather_columns(mixed_out, device_count, 2 * layer + 2)
            whole_rows = post_residual(widened, gathered, post_mixing_multiplier[layer], True)
        else:
            mixed_wide = lax.optimization_barrier(mixed_out).astype(jnp.float32)
            squares = total_over(
                jnp.sum(mixed_wide * mixed_wide, axis=-1), device_count, 2 * layer + 2
            )
            post_rms = lax.rsqrt(squares / D + EPS)[:, None]
            current = (
                own_cols(whole_rows).astype(jnp.float32)
                + mixed_wide * post_rms * own_cols(post_mixing_multiplier[layer])
            ).astype(jnp.bfloat16)
    new_memory = (
        earlier.reshape(layers, batch_total, groups, head_count, LANES)
        .transpose(0, 1, 3, 2, 4)
        .reshape(recurrent_matrices.shape)
    )
    return current.reshape(batch_total, steps, own_width), new_memory


def local_any(*arrays):
    residual_channel, recurrent_matrices = arrays[0], arrays[-1]
    two_heads = (
        recurrent_matrices.shape[2] * HEAD_DIM == LANES
        and residual_channel.shape[1] == 8
        and residual_channel.shape[0] % 16 == 0
        and residual_channel.shape[2] % LANES == 0
        and lax.axis_size("tp") % 4 == 0
        and lax.axis_size("tp") > 4
    )
    return (local_two_heads if two_heads else local)(*arrays)


def solution(mesh):
    return jax.shard_map(
        local_any,
        mesh=mesh,
        in_specs=(
            P("grp", None, "tp"),
            P(),
            P(None, None, "tp"),
            P(None, None, "tp"),
            P(None, None, "tp"),
            P(None, None, "tp"),
            P(),
            P(),
            P(None, "tp"),
            P(None, "tp"),
            P(None, "grp", None, "tp"),
            P(None, "tp"),
            P(None, None, "tp"),
            P(),
            P(None, "grp", "tp", None),
        ),
        out_specs=(P("grp", None, "tp"), P(None, "grp", "tp", None)),
        check_vma=False,
    )
```
